32 devices in a mesh: sp: 16 (over z, y, x), tp: 2 (over core).
Axes of the slice: x: 2, y: 2, z: 4, core: 2. Of those that a mesh axis runs over, the one named last changes fastest.
Arguments:
- stream: bfloat16 [6144, 2048], P('sp'), may hold values from -40 to 40
- query_rows: bfloat16 [6144, 1024], P('sp', 'tp'), may hold values from -10 to 10
- key_rows: bfloat16 [6144, 256], P('sp'), may hold values from -10 to 10
- value_rows: bfloat16 [6144, 256], P('sp'), may hold values from -6 to 6
- doc_ids: int32 [6144], P('sp'), may hold values from 0 to 7, never falling along the last dimension, each value on 1 to 1536 neighbouring positions
- sink_logit: float32 [8], P('tp'), may hold values from 2 to 7
- out_weight: bfloat16 [1024, 2048], P('tp'), may hold values from -1.5 to 1.5
- norm_gain: float32 [2048], replicated, may hold values from 0.1 to 1.9
- gate_weight: bfloat16 [2048, 5632], P('sp', 'tp'), may hold values from -0.125 to 0.125
- up_weight: bfloat16 [2048, 5632], P('sp', 'tp'), may hold values from -0.125 to 0.125
- down_weight: bfloat16 [5632, 2048], P('tp', 'sp'), may hold values from -0.078125 to 0.078125
Outputs:
- mixed_out: bfloat16 [6144, 2048], P('sp')
The draws below stay inside these ranges and needn't reach their ends.
Inputs may be any that keep to these rules, and one draw needn't show every extreme that they name: `doc_ids`: document numbers never fall along the sequence; each document has 1 to 1536 positions.
All inputs are finite; a program needn't handle non-finite values.
Results may differ from the reference program's by a relative error of at most 0.009.
Values may be sent and summed in bfloat16 or wider, within the bound.
A program may use at most 128 MiB of HBM per device.

```python
import math
import jax
import jax.numpy as jnp
import numpy as np
from jax import lax

D = 2048
FF = 5632
HEADS = 8
KVH = 2
HD = 128
WIN = 128
TOK_DEV = 384
TOKENS = 6144
DOCS = 8
DOC_MOST = 1536
N_TP = 2


def draw_stream(key, part):
    first_key, second_key = jax.random.split(key, 2)
    column_scale = 3.0 ** (jnp.arange(D, dtype=jnp.float32) / D)
    base = jnp.clip(jax.random.normal(first_key, (TOKENS, D), jnp.float32), -6.0, 6.0)
    row_scale = jnp.exp(jax.random.uniform(second_key, (TOKENS, 1), jnp.float32, -0.7, 0.7))
    values = base * row_scale * column_scale[None, :]
    return values.astype(jnp.bfloat16)


def draw_query_rows(key, part):
    values = jnp.clip(jax.random.normal(jax.random.fold_in(key, 1), (TOKENS, HEADS * HD), jnp.float32), -6.0, 6.0)
    return values.astype(jnp.bfloat16)


def draw_key_rows(key, part):
    values = jnp.clip(jax.random.normal(jax.random.fold_in(key, 2), (TOKENS, KVH * HD), jnp.float32), -6.0, 6.0)
    return values.astype(jnp.bfloat16)


def block_levels(stream_key, dims, pieces, least, largest):
    def one(dim, blocks):
        heights = jax.random.uniform(jax.random.fold_in(jax.random.fold_in(stream_key, 6), dim), (blocks,), jnp.float32, least / len(pieces), largest / len(pieces))
        return jnp.repeat(jnp.exp(heights), dims[dim] // blocks).reshape((-1,) + (1,) * (len(dims) - dim - 1))

    loudness = one(*pieces[0])
    for cut in pieces[1:]:
        loudness = loudness * one(*cut)
    return loudness


def profile(count, total, reach, slope):
    portions = [(1 << 20) // math.isqrt(rank ** slope) + 1 for rank in range(2, count + 1)]
    surplus, holding = total - reach - (count - 1), [1] * (count - 1)
    while surplus > 0:
        free = [i for i in range(count - 1) if holding[i] < reach]
        whole, remaining = sum([portions[i] for i in free]), surplus
        for i in free:
            more = min(reach - holding[i], max(1, remaining * portions[i] // whole), surplus)
            holding[i] = holding[i] + more
            surplus = surplus - more
    return np.array([reach] + holding)


def uneven_parts(rng, count, total, limit, skew):
    if count == 2:
        one = jax.random.randint(rng, (), max(1, total - limit), min(limit, total - 1) + 1)
        return jnp.stack([one, total - one])
    lengths = jnp.asarray(profile(count, total, limit, skew), jnp.int32)
    couples = (count - 1) // 2
    source_of, sink = lengths[1:1 + 2 * couples:2], lengths[2:2 + 2 * couples:2]
    room = jnp.minimum(source_of - 1, limit - sink)
    passed = jax.random.randint(jax.random.fold_in(rng, 1), (couples,), 0, 1 << 20) % (room + 1)
    lengths = lengths.at[1:1 + 2 * couples:2].set(source_of - passed).at[2:2 + 2 * couples:2].set(sink + passed)
    return lengths[jax.random.permutation(jax.random.fold_in(rng, 2), count)]


def noise(own_key, shape, scale, bound, cuts=(), kind=jnp.bfloat16):
    level = block_levels(own_key, shape, cuts, -0.22, 0.18) if cuts else 1.0
    entries = jax.random.normal(own_key, shape, jnp.float32) * scale * level
    return jnp.minimum(jnp.maximum(entries, -bound), bound).astype(kind)


def setup_inputs(seed: int = 0) -> dict:
    splits = jax.random.split(jax.random.key(seed), 12)
    return {
        "stream": draw_stream(jax.random.fold_in(splits[11], 71), 0),
        "query_rows": draw_query_rows(jax.random.fold_in(splits[11], 71), 0),
        "key_rows": draw_key_rows(jax.random.fold_in(splits[11], 71), 0),
        "value_rows": noise(splits[3], (TOKENS, KVH * HD), 1.0, 6.0, ((0, 16),)),
        "doc_ids": jnp.searchsorted(jnp.cumsum(uneven_parts(splits[4], DOCS, TOKENS, DOC_MOST, 1)), jnp.arange(TOKENS), side="right").astype(jnp.int32),
        "sink_logit": jnp.clip(2.0 + 5.0 * jax.random.uniform(splits[5], (HEADS,), jnp.float32) ** block_levels(splits[5], (HEADS,), ((0, 2),), -0.2, 0.2), 2.0, 7.0),
        "out_weight": noise(splits[6], (HEADS * HD, D), (HEADS * HD // 64) ** -0.5, 1.5, ((0, 2),)),
        "norm_gain": jnp.clip(1.0 + 0.18 * jax.random.normal(splits[7], (D,), jnp.float32), 0.1, 1.9),
        "gate_weight": noise(splits[8], (D, FF), D ** -0.5, 0.125, ((0, 16), (1, 2))),
        "up_weight": noise(splits[9], (D, FF), D ** -0.5, 0.125, ((0, 16), (1, 2))),
        "down_weight": noise(splits[10], (FF, D), FF ** -0.5, 0.078125, ((0, 2), (1, 16))),
    }


norm_eps = 1e-06
masked_low = -1e+30

def reference(stream, query_rows, key_rows, value_rows, doc_ids, sink_logit, out_weight, norm_gain, gate_weight, up_weight, down_weight):
    seq_total = stream.shape[0]
    group_share = HEADS // KVH
    keys_pad = jnp.pad(key_rows, ((WIN, WIN), (0, 0)))
    values_pad = jnp.pad(value_rows, ((WIN, WIN), (0, 0)))
    docs_pad = jnp.pad(doc_ids, (WIN, WIN))
    head_block = HEADS * HD // N_TP
    ff_block = FF // N_TP
    span = TOK_DEV + 2 * WIN

    def one_block(block_id):
        begin_at = (block_id * TOK_DEV).astype(jnp.int32)
        queries = lax.dynamic_slice_in_dim(query_rows, begin_at, TOK_DEV, 0).astype(jnp.float32).reshape(TOK_DEV, KVH, group_share, HD)
        keys_grid = lax.dynamic_slice_in_dim(keys_pad, begin_at, span, 0).astype(jnp.float32).reshape(span, KVH, HD)
        values_grid = lax.dynamic_slice_in_dim(values_pad, begin_at, span, 0).astype(jnp.float32).reshape(span, KVH, HD)
        docs_here = lax.dynamic_slice_in_dim(doc_ids, begin_at, TOK_DEV, 0)
        docs_wide = lax.dynamic_slice_in_dim(docs_pad, begin_at, span, 0)
        query_pos = begin_at + jnp.arange(TOK_DEV, dtype=jnp.int32)
        key_pos = begin_at - WIN + jnp.arange(span, dtype=jnp.int32)
        allowed = (jnp.abs(query_pos[:, None] - key_pos[None, :]) <= WIN) & (key_pos[None, :] >= 0) & (key_pos[None, :] < seq_total) & (docs_here[:, None] == docs_wide[None, :])
        scores = jnp.einsum('qgrd,kgd->grqk', queries, keys_grid) * HD ** (-0.5)
        masked = jnp.where(allowed[None, None], scores, masked_low)
        sinks = sink_logit.astype(jnp.float32).reshape(KVH, group_share, 1, 1)
        peak = jnp.maximum(lax.optimization_barrier(jnp.max(masked, axis=-1, keepdims=True)), sinks)
        lifted = jnp.where(allowed[None, None], jnp.exp(masked - peak), 0.0)
        denom = lax.optimization_barrier(jnp.sum(lifted, axis=-1, keepdims=True)) + jnp.exp(sinks - peak)
        probs = (lifted / denom).astype(jnp.bfloat16)
        attended = jnp.einsum('grqk,kgd->qgrd', probs.astype(jnp.float32), values_grid)
        attended = attended.astype(jnp.bfloat16).reshape(TOK_DEV, HEADS * HD)
        branch_sum = jnp.zeros((TOK_DEV, D), jnp.float32)
        for part_id in range(N_TP):
            term = jnp.dot(attended[:, part_id * head_block:(part_id + 1) * head_block], out_weight[part_id * head_block:(part_id + 1) * head_block], preferred_element_type=jnp.float32)
            branch_sum = branch_sum + lax.optimization_barrier(term.astype(jnp.bfloat16)).astype(jnp.float32)
        branch = branch_sum.astype(jnp.bfloat16)
        stream_here = lax.dynamic_slice_in_dim(stream, begin_at, TOK_DEV, 0)
        carried = (stream_here.astype(jnp.float32) + branch.astype(jnp.float32)).astype(jnp.bfloat16)
        carried_f = carried.astype(jnp.float32)
        normed = (carried_f * lax.rsqrt(lax.optimization_barrier(jnp.mean(carried_f * carried_f, axis=1, keepdims=True)) + norm_eps) * norm_gain.astype(jnp.float32)).astype(jnp.bfloat16)
        gate_acc = jnp.dot(normed, gate_weight, preferred_element_type=jnp.float32)
        up_acc = jnp.dot(normed, up_weight, preferred_element_type=jnp.float32)
        hidden = (jax.nn.silu(gate_acc) * up_acc).astype(jnp.bfloat16)
        feed_sum = jnp.zeros((TOK_DEV, D), jnp.float32)
        for part_id in range(N_TP):
            term = jnp.dot(hidden[:, part_id * ff_block:(part_id + 1) * ff_block], down_weight[part_id * ff_block:(part_id + 1) * ff_block], preferred_element_type=jnp.float32)
            feed_sum = feed_sum + lax.optimization_barrier(term.astype(jnp.bfloat16)).astype(jnp.float32)
        feed = feed_sum.astype(jnp.bfloat16)
        return (carried_f + 0.5 * feed.astype(jnp.float32)).astype(jnp.bfloat16)
    blocks_all = lax.map(one_block, jnp.arange(seq_total // TOK_DEV, dtype=jnp.int32))
    return blocks_all.reshape(seq_total, D)
```

```python
import jax
import jax.numpy as jnp
from jax import lax
from jax.sharding import Mesh, PartitionSpec as P

HEADS = 8
KVH = 2
HD = 128
WIN = 128

norm_eps = 1e-06
masked_low = -1e30
SP = ("sa", "sb")


def halo(value, width):
    peers = lax.axis_size(SP)
    length = value.shape[0]
    up = [(i, i + 1) for i in range(peers - 1)]
    down = [(j, i) for i, j in up]
    before = lax.ppermute(value[length - width :], SP, up)
    after = lax.ppermute(value[:width], SP, down)
    return jnp.concatenate([before, value, after], axis=0)


def exchange(blocks):
    peers = lax.axis_size("sa")
    here = lax.axis_index("sa")
    got = [lax.dynamic_index_in_dim(blocks, here, 0, keepdims=True)]
    for k in range(1, peers):
        out = lax.dynamic_index_in_dim(blocks, lax.rem(here + k, peers), 0, keepdims=True)
        got.append(lax.ppermute(out, "sa", [(i, (i + k) % peers) for i in range(peers)]))
    ring = got[::-1]
    both = jnp.concatenate(ring + ring, axis=0)
    return lax.dynamic_slice_in_dim(both, peers - 1 - here, peers, 0)


def per_device(
    stream,
    query_rows,
    key_rows,
    value_rows,
    doc_ids,
    sink_logit,
    out_weight,
    norm_gain,
    gate_weight,
    up_weight,
    down_weight,
):
    row_count, width = stream.shape
    n_a, n_b, n_tp = lax.axis_size("sa"), lax.axis_size("sb"), lax.axis_size("tp")
    depth, hidden_here = gate_weight.shape
    share = hidden_here // n_a
    tp_place = lax.axis_index("tp")
    sp_place = lax.axis_index(SP)

    def shares(w):
        return w.reshape(depth, n_a, share).transpose(1, 0, 2)

    gate_up = exchange(jnp.concatenate([shares(gate_weight), shares(up_weight)], axis=2))
    gate_up = gate_up.reshape(n_a * depth, 2 * share)
    gate_up = lax.all_gather(gate_up, "sb", axis=0, tiled=True)
    down_mine = exchange(down_weight.reshape(n_a, share, depth))
    down_mine = down_mine.transpose(0, 2, 1).reshape(n_a * depth, share)

    heads_here = query_rows.shape[1] // HD
    group_share = HEADS // KVH
    groups_here = max(1, heads_here // group_share)
    per_group = heads_here // groups_here
    group_first = tp_place * heads_here // group_share
    keys_here = lax.dynamic_slice_in_dim(key_rows, group_first * HD, groups_here * HD, 1)
    values_here = lax.dynamic_slice_in_dim(value_rows, group_first * HD, groups_here * HD, 1)
    docs_col = jnp.broadcast_to(doc_ids.astype(jnp.bfloat16)[:, None], (row_count, HD))
    packed = halo(jnp.concatenate([keys_here, values_here, docs_col], axis=1), WIN)
    span = groups_here * HD
    keys_wide, values_wide = packed[:, :span], packed[:, span : 2 * span]
    docs_wide = packed[:, 2 * span].astype(jnp.int32)
    seq_offset = sp_place * row_count
    seq_total = row_count * n_a * n_b
    query_pos = seq_offset + jnp.arange(row_count, dtype=jnp.int32)
    key_pos = seq_offset - WIN + jnp.arange(row_count + 2 * WIN, dtype=jnp.int32)
    allowed = (
        (jnp.abs(query_pos[:, None] - key_pos[None, :]) <= WIN)
        & (key_pos[None, :] >= 0)
        & (key_pos[None, :] < seq_total)
        & (doc_ids[:, None] == docs_wide[None, :])
    )
    queries = query_rows.reshape(row_count, groups_here, per_group, HD)
    keys_grid = keys_wide.reshape(row_count + 2 * WIN, groups_here, HD)
    values_grid = values_wide.reshape(row_count + 2 * WIN, groups_here, HD)
    scores = jnp.einsum(
        "qgrd,kgd->grqk", queries, keys_grid, preferred_element_type=jnp.float32
    ) * HD ** (-0.5)
    masked = jnp.where(allowed[None, None], scores, masked_low)
    sinks = sink_logit.reshape(groups_here, per_group, 1, 1)
    peak = jnp.maximum(jnp.max(masked, axis=-1, keepdims=True), sinks)
    lifted = jnp.where(allowed[None, None], jnp.exp(masked - peak), 0.0)
    denom = jnp.sum(lifted, axis=-1, keepdims=True) + jnp.exp(sinks - peak)
    probs = (lifted / denom).astype(jnp.bfloat16)
    attended = jnp.einsum("grqk,kgd->qgrd", probs, values_grid, preferred_element_type=jnp.float32)
    attended = attended.astype(jnp.bfloat16).reshape(row_count, heads_here * HD)
    partial_value = jnp.dot(attended, out_weight, preferred_element_type=jnp.float32)

    rows_mine = row_count // n_tp
    branch = lax.psum_scatter(
        partial_value.astype(jnp.bfloat16), "tp", scatter_dimension=0, tiled=True
    )
    stream_mine = lax.dynamic_slice_in_dim(stream, tp_place * rows_mine, rows_mine, 0)
    carried = (stream_mine.astype(jnp.float32) + branch.astype(jnp.float32)).astype(jnp.bfloat16)
    carried_f = carried.astype(jnp.float32)
    normed = (
        carried_f
        * lax.rsqrt(jnp.mean(carried_f * carried_f, axis=1, keepdims=True) + norm_eps)
        * norm_gain[None, :]
    ).astype(jnp.bfloat16)
    normed = normed.reshape(rows_mine, n_a, n_b, depth).transpose(0, 2, 1, 3).reshape(rows_mine, width)
    rows_all = lax.all_gather(normed, ("sa", "tp"), axis=0, tiled=True)
    down_mine, _ = lax.optimization_barrier((down_mine, normed))
    down_all = lax.all_gather(down_mine, "sb", axis=0, tiled=True)

    gate_acc = jnp.dot(rows_all, gate_up[:, :share], preferred_element_type=jnp.float32)
    up_acc = jnp.dot(rows_all, gate_up[:, share:], preferred_element_type=jnp.float32)
    hidden = (jax.nn.silu(gate_acc) * up_acc).astype(jnp.bfloat16)
    terms = lax.dot_general(
        hidden, down_all, (((1,), (1,)), ((), ())), preferred_element_type=jnp.float32
    )
    feed = lax.psum_scatter(
        terms.astype(jnp.bfloat16), ("sa", "tp"), scatter_dimension=0, tiled=True
    )
    feed = feed.reshape(rows_mine, n_b, n_a, depth).transpose(0, 2, 1, 3).reshape(rows_mine, width)
    mixed = (carried_f + 0.5 * feed.astype(jnp.float32)).astype(jnp.bfloat16)
    return lax.all_gather(mixed, "tp", axis=0, tiled=True)


def solution(mesh):
    n_sp, n_tp = mesh.shape["sp"], mesh.shape["tp"]
    n_a = 4 if n_sp % 4 == 0 else 1
    fine = Mesh(mesh.devices.reshape(n_a, n_sp // n_a, n_tp), ("sa", "sb", "tp"))
    in_specs = (
        P(SP, None),
        P(SP, "tp"),
        P(SP, None),
        P(SP, None),
        P(SP),
        P("tp"),
        P("tp", None),
        P(),
        P(SP, "tp"),
        P(SP, "tp"),
        P("tp", SP),
    )
    return jax.shard_map(
        per_device, mesh=fine, in_specs=in_specs, out_specs=P(SP, None), check_vma=False
    )
```
